32 devices in a mesh: grp: 2 (over y), ep: 4 (over z), tp: 4 (over x, core).
Axes of the slice: x: 2, y: 2, z: 4, core: 2. Of those that a mesh axis runs over, the one named last changes fastest.
Arguments:
- mix_input: bfloat16 [2048, 2048], P(('grp', 'ep'), 'tp'), parts along dimension 0, may hold values from -6 to 6
- group_weight: bfloat16 [16, 128, 128], replicated, may hold values from -0.5 to 0.5
- pool_gain: float32 [2048], replicated, may hold values from 0.1 to 1.9
- branch_weight: bfloat16 [2048, 2048], P('tp'), may hold values from -0.125 to 0.125
- exp_input: bfloat16 [1024, 2048], P(('grp', 'ep')), parts along dimension 0, may hold values from -6 to 6
- norm_gain: float32 [2048], replicated, may hold values from 0.1 to 1.9
- routes: int32 [1024, 2], P(('grp', 'ep')), parts along dimension 0, may hold values from 0 to 3, all different within a row; in each aligned block of 128 rows (0 to 127, 128 to 255, ...) at most 96 rows name the same one
- route_weights: float32 [1024, 2], P(('grp', 'ep')), parts along dimension 0, may hold values from 0.25 to 1
- gate_weight: bfloat16 [4, 2048, 3584], P('ep', None, 'tp'), may hold values from -0.125 to 0.125
- up_weight: bfloat16 [4, 2048, 3584], P('ep', None, 'tp'), may hold values from -0.125 to 0.125
- down_weight: bfloat16 [4, 3584, 2048], P('ep', 'tp'), may hold values from -0.09375 to 0.09375
Outputs:
- mix_out: bfloat16 [2048, 2048], P(('grp', 'ep'), 'tp'), parts along dimension 0
- exp_out: bfloat16 [1024, 2048], P(('grp', 'ep'), 'tp'), parts along dimension 0
The draws below stay inside these ranges and needn't reach their ends.
There are 2 independent parts, one for each index of `grp`. The reference program is written for one: setup_inputs(seed, part) draws one part's arguments, and reference() takes and returns one part's arrays. A program takes and returns all parts, laid end to end along the dimension named above; an argument that names none is the same for every part. Nothing has to cross between parts.
Inputs may be any that keep to these rules, and one draw needn't show every extreme that they name: `routes`: the 2 experts of a token differ. Among the 128 tokens of one index of ep no expert is named by more than 96 of them, a bound that some block reaches.
All inputs are finite; a program needn't handle non-finite values.
Results may differ from the reference program's by a relative error of at most 0.018.
Values may be sent and summed in bfloat16 or wider, within the bound.
No kernel may reach another device: no remote copies, remote signals or barrier semaphores. Data moves between devices by JAX's collectives and lax.ppermute only.
A program may use at most 64 MiB of HBM per device.

```python
import math
import jax
import jax.numpy as jnp
import numpy as np
from jax import lax

WIDTH = 2048
GROUPS = 16
GROUP_WIDTH = 128
HIDDEN_SIZE = 3584
TOP_K = 2
TOK_EXP = 128
POOL_WIDTH = 2048
EXPERTS = 4
MIX_TOKENS = 1024
EXP_TOKENS = 512
EXP_ROWS = 384
CAP_SLOTS = 96
N_TP = 4


def steps_of(rng, dims, shards, smallest, largest):
    loudness, own = 1.0, jax.random.fold_in(rng, 6)
    for position, shards_of in shards:
        steps = jnp.exp(jax.random.uniform(jax.random.fold_in(own, position), (shards_of,), jnp.float32, smallest / len(shards), largest / len(shards)))
        loudness = loudness * jnp.repeat(steps, dims[position] // shards_of).reshape([-1 if axis == position else 1 for axis in range(len(dims))])
    return loudness


def assign_block(rng, own, number, rows, count, top, bound, slope):
    order = jax.random.permutation(rng, count)
    heavy_load, ordinary = load_shares(count, rows * top, bound, slope, True), load_shares(count, rows * top, bound, slope, False)
    places = jnp.arange(count)

    def named(sizes, offset_by):
        used = int((sizes > 0).sum())
        fixed = max(1, used // 4)
        passed = fixed + (places - fixed + offset_by * (used - fixed)) % max(1, count - fixed)
        return jnp.zeros((count,), jnp.int32).at[order[jnp.where(places < fixed, places, passed)]].set(jnp.asarray(sizes, jnp.int32))

    sizes = jnp.where(number % 4 == 0, named(heavy_load, number // 4), named(ordinary, number - number // 4 - 1))
    mixed = jax.random.permutation(jax.random.fold_in(own, 3), count)
    giver, sink = mixed[0:count // 2 * 2:2], mixed[1:count // 2 * 2:2]
    room = jnp.minimum(sizes[giver] - 1, bound - sizes[sink]) // 2
    room = jnp.where((giver == order[0]) | (sink == order[0]) | (sizes[sink] == 0), 0, jnp.maximum(room, 0))
    passed = jax.random.randint(jax.random.fold_in(own, 4), (count // 2,), 0, 1 << 20) % (room + 1)
    sizes = sizes.at[giver].add(-passed).at[sink].add(passed)
    labels = jnp.searchsorted(jnp.cumsum(sizes), jnp.arange(rows * top), side="right").astype(jnp.int32)
    grid = labels.reshape(top, rows).T
    grid = grid[jax.random.permutation(jax.random.fold_in(own, 1), rows)]
    offset_by = jax.random.randint(jax.random.fold_in(own, 2), (rows, 1), 0, top)
    return jnp.take_along_axis(grid, (jnp.arange(top)[None, :] + offset_by) % top, axis=1)


def load_shares(count, total, limit, skew, full):
    weights = [(1 << 20) // math.isqrt(standing ** skew) + 1 for standing in range(1, count + 1)]
    largest = limit if full else min(limit, max(-(-total // count), total * weights[0] // sum(weights)))
    least = 1 if total - largest >= count - 1 else 0
    given, spare = [largest] + [least] * (count - 1), total - largest - least * (count - 1)
    while spare > 0:
        free = [i for i in range(1, count) if given[i] < largest] or [i for i in range(1, count) if given[i] < limit]
        mass, budget = sum([weights[i] for i in free]), spare
        for i in free:
            more = min(limit - given[i], max(1, budget * weights[i] // mass), spare)
            given[i] = given[i] + more
            spare = spare - more
    return np.array(given)


def gaussian(rng, shape, spread, bound, split=(), kind=jnp.bfloat16):
    drawn = spread * jax.random.normal(rng, shape, jnp.float32)
    if split:
        drawn = drawn * steps_of(rng, shape, split, -0.22, 0.18)
    return jnp.clip(drawn, -bound, bound).astype(kind)


def setup_inputs(seed: int = 0, part: int = 0) -> dict:
    key_list = jax.random.split(jax.random.key(seed), 12)
    own_keys = jax.random.split(jax.random.fold_in(key_list[11], part), 12)
    mix_input = gaussian(own_keys[0], (MIX_TOKENS, POOL_WIDTH), 1.0, 6.0, ((0, 4), (1, 4)))
    group_weight = gaussian(key_list[1], (GROUPS, GROUP_WIDTH, GROUP_WIDTH), GROUP_WIDTH ** -0.5, 0.5)
    pool_gain = jnp.clip(1.0 + 0.18 * jax.random.normal(key_list[2], (POOL_WIDTH,), jnp.float32), 0.1, 1.9)
    branch_weight = gaussian(key_list[3], (POOL_WIDTH, WIDTH), POOL_WIDTH ** -0.5, 0.125, ((0, 4),))
    exp_input = gaussian(own_keys[4], (EXP_TOKENS, WIDTH), 1.0, 6.0, ((0, 4),))
    norm_gain = jnp.clip(1.0 + 0.18 * jax.random.normal(key_list[5], (WIDTH,), jnp.float32), 0.1, 1.9)
    routes_keys = jax.random.split(jax.random.fold_in(own_keys[6], 1), EXP_TOKENS // TOK_EXP)
    routes_turns = jax.random.permutation(jax.random.fold_in(own_keys[6], 3), EXP_TOKENS // TOK_EXP)
    routes = jax.vmap(lambda own, number: assign_block(jax.random.fold_in(own_keys[6], 2), own, number, TOK_EXP, EXPERTS, TOP_K, CAP_SLOTS, 1))(routes_keys, routes_turns).reshape((EXP_TOKENS, TOP_K))
    route_weights = jnp.clip(0.25 + 0.75 * jax.random.uniform(own_keys[7], (EXP_TOKENS, TOP_K), jnp.float32) ** steps_of(own_keys[7], (EXP_TOKENS, TOP_K), ((0, 4),), -0.2, 0.2), 0.25, 1.0)
    gate_weight = gaussian(key_list[8], (EXPERTS, WIDTH, HIDDEN_SIZE), WIDTH ** -0.5, 0.125, ((0, 4), (2, 4)))
    up_weight = gaussian(key_list[9], (EXPERTS, WIDTH, HIDDEN_SIZE), WIDTH ** -0.5, 0.125, ((0, 4), (2, 4)))
    down_weight = gaussian(key_list[10], (EXPERTS, HIDDEN_SIZE, WIDTH), HIDDEN_SIZE ** -0.5, 0.09375, ((0, 4), (1, 4)))
    return dict(mix_input=mix_input, group_weight=group_weight, pool_gain=pool_gain, branch_weight=branch_weight, exp_input=exp_input, norm_gain=norm_gain, routes=routes, route_weights=route_weights, gate_weight=gate_weight, up_weight=up_weight, down_weight=down_weight)


windows = (2, 4, 8, 16)
epsilon = 1e-06

def trailing_sums(extended, rows):
    span_two = extended[1:] + extended[:-1]
    span_four = span_two[2:] + span_two[:-2]
    span_eight = span_four[4:] + span_four[:-4]
    span_sixteen = span_eight[8:] + span_eight[:-8]
    return [span_two[-rows:], span_four[-rows:], span_eight[-rows:], span_sixteen[-rows:]]

def pooled_deviation(extended, positions, group_ids, group_width, rows):
    sums = trailing_sums(extended, rows)
    current = extended[-rows:]
    window_id = jnp.repeat(group_ids % 4, group_width)
    result = jnp.zeros_like(current)
    for window_level, window_len in enumerate(windows):
        counted = jnp.minimum(positions + 1, window_len).astype(jnp.float32)[:, None]
        result = jnp.where(window_id[None, :] == window_level, sums[window_level] / counted - current, result)
    return result

def blockwise_product(left, right, blocks):
    inner = left.shape[1] // blocks
    left_pieces = left.reshape(left.shape[0], blocks, inner).transpose(1, 0, 2)
    right_pieces = right.reshape(blocks, inner, right.shape[1])

    def add_block(running, operands):
        piece, weight = operands
        rounded = lax.optimization_barrier(jnp.dot(piece, weight, preferred_element_type=jnp.float32).astype(jnp.bfloat16))
        return (running + rounded.astype(jnp.float32), None)
    start_sum = jnp.zeros((left.shape[0], right.shape[1]), jnp.float32)
    running, _ = lax.scan(add_block, start_sum, (left_pieces, right_pieces))
    return running.astype(jnp.bfloat16)

def reference(mix_input, group_weight, pool_gain, branch_weight, exp_input, norm_gain, routes, route_weights, gate_weight, up_weight, down_weight):
    rows = mix_input.shape[0]
    extended = jnp.concatenate([jnp.zeros((15, POOL_WIDTH), jnp.float32), mix_input.astype(jnp.float32)], axis=0)
    positions = jnp.arange(rows, dtype=jnp.int32)
    group_ids = jnp.arange(GROUPS, dtype=jnp.int32)
    deviation = pooled_deviation(extended, positions, group_ids, GROUP_WIDTH, rows).astype(jnp.bfloat16)
    grouped = jnp.einsum('rgc,gcd->rgd', deviation.reshape(rows, GROUPS, GROUP_WIDTH).astype(jnp.float32), group_weight.astype(jnp.float32)).reshape(rows, POOL_WIDTH)
    pooled = (grouped * pool_gain).astype(jnp.bfloat16)
    mix_out = blockwise_product(pooled, branch_weight, N_TP)
    tokens = exp_input.shape[0]
    floated = exp_input.astype(jnp.float32)
    normed = (floated * lax.rsqrt(lax.optimization_barrier(jnp.mean(floated * floated, axis=1, keepdims=True)) + epsilon) * norm_gain).astype(jnp.bfloat16)
    flat_expert = routes.reshape(-1).astype(jnp.int32)
    assignments = flat_expert.shape[0]
    onehot = (flat_expert[:, None] == jnp.arange(EXPERTS, dtype=jnp.int32)[None, :]).astype(jnp.int32)
    slot_rank = lax.optimization_barrier(jnp.sum((jnp.cumsum(onehot, axis=0) - onehot) * onehot, axis=1)).astype(jnp.int32)
    token_of = (jnp.arange(assignments, dtype=jnp.int32) // TOP_K).astype(jnp.int32)
    slot_table = jnp.full((EXPERTS, EXP_ROWS), tokens, jnp.int32).at[flat_expert, slot_rank].set(token_of)
    padded = jnp.concatenate([normed, jnp.zeros((1, WIDTH), jnp.bfloat16)], axis=0)

    def one_expert(operands):
        row_index, w_gate, w_up, w_down = operands
        chosen = padded[row_index]
        gate_pre = jnp.dot(chosen, w_gate, preferred_element_type=jnp.float32)
        up_pre = jnp.dot(chosen, w_up, preferred_element_type=jnp.float32)
        hidden = (jax.nn.silu(gate_pre) * up_pre).astype(jnp.bfloat16)
        return blockwise_product(hidden, w_down, N_TP)
    outputs = lax.map(one_expert, (slot_table, gate_weight, up_weight, down_weight))
    picked = outputs[flat_expert, slot_rank].astype(jnp.float32).reshape(tokens, TOP_K, WIDTH)
    exp_out = lax.optimization_barrier(jnp.sum(picked * route_weights[:, :, None], axis=1)).astype(jnp.bfloat16)
    return (mix_out, exp_out)
```

```python
import jax
import jax.numpy as jnp
from jax import lax
from jax.sharding import PartitionSpec as P

windows = (2, 4, 8, 16)
epsilon = 1e-06


def shifted(block, axis, distance):
    devices = range(lax.axis_size(axis))
    route = [(i - distance, i) for i in devices if i - distance in devices]
    return lax.ppermute(block, axis, route)


def rotated(block, axis, distance):
    count = lax.axis_size(axis)
    return lax.ppermute(block, axis, [(i, (i + distance) % count) for i in range(count)])


def paired(block):
    count = lax.axis_size("tp")
    return lax.ppermute(block, "tp", [(i, i ^ 1) for i in range(count)])


def trailing_sums(extended, rows):
    span_two = extended[1:] + extended[:-1]
    span_four = span_two[2:] + span_two[:-2]
    span_eight = span_four[4:] + span_four[:-4]
    span_sixteen = span_eight[8:] + span_eight[:-8]
    return [span_two[-rows:], span_four[-rows:], span_eight[-rows:], span_sixteen]


def pooled_deviation(extended, positions, group_ids, group_width, rows):
    sums = trailing_sums(extended, rows)
    current = extended[-rows:]
    window_id = jnp.repeat(group_ids % 4, group_width)
    result = jnp.zeros_like(current)
    for window_level, window_len in enumerate(windows):
        counted = jnp.minimum(positions + 1, window_len).astype(jnp.float32)[:, None]
        result = jnp.where(
            window_id[None, :] == window_level, sums[window_level] / counted - current, result
        )
    return result


def scattered(partial, tp_rank):
    rows, width = partial.shape
    members = lax.axis_size("tp")
    chips = members // 2
    columns = width // members
    core, chip = tp_rank % 2, tp_rank // 2
    blocks = partial.reshape(rows, chips, 2, columns)
    keep = lax.dynamic_index_in_dim(blocks, core, 2, keepdims=False)
    give = lax.dynamic_index_in_dim(blocks, 1 - core, 2, keepdims=False)
    got = paired(give)
    half = (keep.astype(jnp.float32) + got.astype(jnp.float32)).astype(jnp.bfloat16)
    total = lax.dynamic_index_in_dim(half, chip, 1, keepdims=False).astype(jnp.float32)
    for step in range(1, chips):
        target = (chip + step) % chips
        piece = lax.dynamic_index_in_dim(half, target, 1, keepdims=False)
        total = total + rotated(piece, "tp", 2 * step).astype(jnp.float32)
    return total.astype(jnp.bfloat16)


def on_device(
    mix_input,
    group_weight,
    pool_gain,
    branch_weight,
    exp_input,
    norm_gain,
    routes,
    route_weights,
    gate_weight,
    up_weight,
    down_weight,
):
    tp_rank = lax.axis_index("tp")
    ep_rank = lax.axis_index("ep")
    experts_all = lax.axis_size("ep")
    core = tp_rank % 2
    tok_rows, width = exp_input.shape
    capacity = 3 * tok_rows // experts_all
    floated = exp_input.astype(jnp.float32)
    normed = (
        floated
        * lax.rsqrt(jnp.mean(floated * floated, axis=1, keepdims=True) + epsilon)
        * norm_gain
    ).astype(jnp.bfloat16)
    half_width = width // 2
    normed_half = lax.dynamic_slice_in_dim(normed, core * half_width, half_width, 1)
    relative = (ep_rank + jnp.arange(experts_all, dtype=jnp.int32)) % experts_all
    choice = routes[:, :, None] == relative[None, None, :]
    member = jnp.any(choice, axis=1)
    member_t = jnp.any(routes.T[:, None, :] == relative[None, :, None], axis=0)
    before = jnp.arange(tok_rows)[:, None] < jnp.arange(tok_rows)[None, :]
    rank_t = jnp.dot(
        member_t.astype(jnp.bfloat16), before.astype(jnp.bfloat16), preferred_element_type=jnp.float32
    ).astype(jnp.int32)
    slots = jnp.arange(capacity, dtype=jnp.int32)
    select = (
        member_t[:, None, :] & (rank_t[:, None, :] == slots[None, :, None])
    ).astype(jnp.bfloat16)
    outgoing = jnp.dot(
        select[1:].reshape((experts_all - 1) * capacity, tok_rows),
        normed_half,
        preferred_element_type=jnp.float32,
    ).astype(jnp.bfloat16)
    own_rows = jnp.dot(select[0], normed, preferred_element_type=jnp.float32).astype(jnp.bfloat16)
    arrivals = [
        rotated(outgoing[(k - 1) * capacity : k * capacity], "ep", k) for k in range(1, experts_all)
    ]
    rows_mix, channels = mix_input.shape
    group_width = group_weight.shape[1]
    group_count = channels // group_width
    first_group = tp_rank * group_count
    before_rows = shifted(mix_input[rows_mix - 15 :], "ep", 1)
    extended = jnp.concatenate([before_rows, mix_input], axis=0).astype(jnp.float32)
    positions = ep_rank * rows_mix + jnp.arange(rows_mix, dtype=jnp.int32)
    group_ids = first_group + jnp.arange(group_count, dtype=jnp.int32)
    deviation = pooled_deviation(extended, positions, group_ids, group_width, rows_mix).astype(
        jnp.bfloat16
    )
    own_groups = lax.dynamic_slice_in_dim(group_weight, first_group, group_count, 0)
    grouped = jnp.concatenate(
        [
            jnp.dot(
                deviation[:, g * group_width : (g + 1) * group_width],
                own_groups[g],
                preferred_element_type=jnp.float32,
            )
            for g in range(group_count)
        ],
        axis=1,
    )
    own_gain = lax.dynamic_slice_in_dim(pool_gain, first_group * group_width, channels, 0)
    pooled = (grouped * own_gain).astype(jnp.bfloat16)
    mix_partial = jnp.dot(pooled, branch_weight, preferred_element_type=jnp.float32).astype(
        jnp.bfloat16
    )
    mix_out = scattered(mix_partial, tp_rank)
    mine = jnp.concatenate(arrivals, axis=0)
    theirs = paired(mine)
    is_low = core == 0
    section = jnp.concatenate(
        [
            own_rows,
            jnp.concatenate(
                [jnp.where(is_low, mine, theirs), jnp.where(is_low, theirs, mine)], axis=1
            ),
        ],
        axis=0,
    )
    gate_pre = jnp.dot(section, gate_weight[0], preferred_element_type=jnp.float32)
    up_pre = jnp.dot(section, up_weight[0], preferred_element_type=jnp.float32)
    hidden = (jax.nn.silu(gate_pre) * up_pre).astype(jnp.bfloat16)
    down = jnp.dot(hidden, down_weight[0], preferred_element_type=jnp.float32).astype(jnp.bfloat16)
    results = scattered(down, tp_rank)
    returned = [results[:capacity]] + [
        rotated(results[k * capacity : (k + 1) * capacity], "ep", -k) for k in range(1, experts_all)
    ]
    returned = jnp.concatenate(returned, axis=0)
    rank = rank_t.T
    exp_out = jnp.zeros((tok_rows, results.shape[1]), jnp.float32)
    for k in range(routes.shape[1]):
        pick = choice[:, k, :, None] & (rank[:, :, None] == slots[None, None, :])
        pick = pick.reshape(tok_rows, experts_all * capacity).astype(jnp.bfloat16)
        chosen = jnp.dot(pick, returned, preferred_element_type=jnp.float32)
        exp_out = exp_out + chosen * route_weights[:, k : k + 1]
    return (mix_out, exp_out.astype(jnp.bfloat16))


def solution(mesh):
    return jax.shard_map(
        on_device,
        mesh=mesh,
        in_specs=(
            P(("grp", "ep"), "tp"),
            P(),
            P(),
            P("tp", None),
            P(("grp", "ep"), None),
            P(),
            P(("grp", "ep"), None),
            P(("grp", "ep"), None),
            P("ep", None, "tp"),
            P("ep", None, "tp"),
            P("ep", "tp", None),
        ),
        out_specs=(P(("grp", "ep"), "tp"), P(("grp", "ep"), "tp")),
        check_vma=False,
    )
```

```python
import jax
import jax.numpy as jnp
from jax import lax
from jax.experimental import pallas as pl
from jax.experimental.pallas import tpu as pltpu
from jax.sharding import PartitionSpec as P

windows = (2, 4, 8, 16)
epsilon = 1e-06
halo = 16
f32, bf16 = jnp.float32, jnp.bfloat16


def shifted(block, axis, distance):
    devices = range(lax.axis_size(axis))
    route = [(i - distance, i) for i in devices if i - distance in devices]
    return lax.ppermute(block, axis, route)


def rotated(block, axis, distance):
    count = lax.axis_size(axis)
    return lax.ppermute(block, axis, [(i, (i + distance) % count) for i in range(count)])


def paired(block):
    count = lax.axis_size("tp")
    return lax.ppermute(block, "tp", [(i, i ^ 1) for i in range(count)])


def ranks_of(routes, ep_rank, experts):
    tokens, top = routes.shape
    relative = lax.rem(ep_rank + lax.broadcasted_iota(jnp.int32, (tokens, experts), 1), experts)
    hits = [(routes[:, k : k + 1] == relative) for k in range(top)]
    member = sum(jnp.where(h, 1.0, 0.0) for h in hits)
    row = lax.broadcasted_iota(jnp.int32, (tokens, tokens), 0)
    col = lax.broadcasted_iota(jnp.int32, (tokens, tokens), 1)
    before = jnp.where(col < row, 1.0, 0.0).astype(bf16)
    rank = jnp.dot(before, member.astype(bf16), preferred_element_type=f32)
    return [jnp.where(h, rank, -1.0) for h in hits], jnp.where(member > 0.5, rank, -1.0)


def prepare(scalars, exp_input, norm_gain, routes, order, capacity):
    tokens, width = exp_input.shape
    half = width // 2
    experts = len(order)

    def body(scal, x_ref, gain_ref, routes_ref, *outs):
        floated = x_ref[...].astype(f32)
        scale = lax.rsqrt(jnp.mean(floated * floated, axis=1, keepdims=True) + epsilon)
        low = (floated[:, :half] * scale * gain_ref[:, :half]).astype(bf16)
        high = (floated[:, half:] * scale * gain_ref[:, half:]).astype(bf16)
        mine = jnp.where(lax.rem(scal[0], 2) == 0, low, high)
        _, place = ranks_of(routes_ref[...], scal[1], experts)
        slots = lax.broadcasted_iota(jnp.int32, (tokens, capacity), 1).astype(f32)
        for out, k in zip(outs, order):
            pick = jnp.where(place[:, k : k + 1] == slots, 1.0, 0.0).astype(bf16)
            out[...] = lax.dot_general(
                pick, mine, (((0,), (0,)), ((), ())), preferred_element_type=f32
            ).astype(bf16)

    return pl.pallas_call(
        body,
        in_specs=[
            pl.BlockSpec(memory_space=pltpu.SMEM),
            pl.BlockSpec(memory_space=pltpu.VMEM),
            pl.BlockSpec(memory_space=pltpu.VMEM),
            pl.BlockSpec(memory_space=pltpu.VMEM),
        ],
        out_specs=[pl.BlockSpec(memory_space=pltpu.VMEM)] * experts,
        out_shape=[jax.ShapeDtypeStruct((capacity, half), bf16)] * experts,
        name="prepare",
    )(scalars, exp_input, norm_gain.reshape(1, width), routes)


def combine(scalars, routes, route_weights, chunks, order):
    tokens, top = routes.shape
    capacity, columns = chunks[0].shape
    experts = len(order)

    def body(scal, routes_ref, weights_ref, *refs):
        out = refs[-1]
        places, _ = ranks_of(routes_ref[...], scal[1], experts)
        slots = lax.broadcasted_iota(jnp.int32, (tokens, capacity), 1).astype(f32)
        total = jnp.zeros((tokens, columns), f32)
        for k in range(top):
            chosen = jnp.zeros((tokens, columns), f32)
            for ref, e in zip(refs, order):
                pick = jnp.where(places[k][:, e : e + 1] == slots, 1.0, 0.0).astype(bf16)
                chosen = chosen + jnp.dot(pick, ref[...], preferred_element_type=f32)
            total = total + chosen * weights_ref[:, k : k + 1]
        out[...] = total.astype(bf16)

    return pl.pallas_call(
        body,
        in_specs=[pl.BlockSpec(memory_space=pltpu.SMEM)]
        + [pl.BlockSpec(memory_space=pltpu.VMEM)] * (2 + experts),
        out_specs=pl.BlockSpec(memory_space=pltpu.VMEM),
        out_shape=jax.ShapeDtypeStruct((tokens, columns), bf16),
        name="combine",
    )(scalars, routes, route_weights, *chunks)


def column_block(step, rank, chips):
    core, chip = lax.rem(rank, 2), lax.div(rank, 2)
    place = lax.rem(chip + lax.rem(step, chips), chips)
    return 2 * place + jnp.where(step < chips, 1 - core, core)


def mixer(scalars, mix_input, before, group_weight, pool_gain, branch_weight, members):
    rows, channels = mix_input.shape
    group_width = group_weight.shape[1]
    group_count = channels // group_width
    width = branch_weight.shape[1]
    columns = width // members
    chips = members // 2

    def body(scal, x_ref, before_ref, group_ref, gain_ref, branch_ref, give_ref, keep_ref, pooled):
        step = pl.program_id(0)

        @pl.when(step == 0)
        def _():
            place = scal[1] * rows + lax.broadcasted_iota(jnp.int32, (rows, group_width), 0)
            for g in range(group_count):
                cut = slice(g * group_width, (g + 1) * group_width)
                extended = jnp.concatenate(
                    [before_ref[:, cut].astype(f32), x_ref[:, cut].astype(f32)], axis=0
                )
                level = lax.rem(scal[0] * group_count + g, len(windows))
                sums = extended
                chosen = jnp.zeros_like(extended)
                for index, window in enumerate(windows):
                    sums = sums + pltpu.roll(sums, window // 2, 0)
                    chosen = jnp.where(level == index, sums, chosen)
                length = lax.shift_left(jnp.int32(2), level)
                counted = jnp.minimum(place + 1, length).astype(f32)
                deviation = (chosen[halo:] / counted - extended[halo:]).astype(bf16)
                grouped = jnp.dot(deviation, group_ref[g], preferred_element_type=f32)
                pooled[:, cut] = (grouped * gain_ref[:, cut]).astype(bf16)

        result = jnp.dot(pooled[...], branch_ref[...], preferred_element_type=f32).astype(bf16)

        @pl.when(step < chips)
        def _():
            give_ref[0] = result

        @pl.when(step >= chips)
        def _():
            keep_ref[0] = result

    return pl.pallas_call(
        body,
        grid_spec=pltpu.PrefetchScalarGridSpec(
            num_scalar_prefetch=1,
            grid=(members,),
            in_specs=[
                pl.BlockSpec((rows, channels), lambda i, s: (0, 0)),
                pl.BlockSpec((halo, channels), lambda i, s: (0, 0)),
                pl.BlockSpec((group_count, group_width, group_width), lambda i, s: (s[0], 0, 0)),
                pl.BlockSpec((1, channels), lambda i, s: (0, s[0])),
                pl.BlockSpec((channels, columns), lambda i, s: (0, column_block(i, s[0], chips))),
            ],
            out_specs=[
                pl.BlockSpec((1, rows, columns), lambda i, s: (jnp.minimum(i, chips - 1), 0, 0)),
                pl.BlockSpec((1, rows, columns), lambda i, s: (jnp.maximum(i - chips, 0), 0, 0)),
            ],
            scratch_shapes=[pltpu.VMEM((rows, channels), bf16)],
        ),
        out_shape=[jax.ShapeDtypeStruct((chips, rows, columns), bf16)] * 2,
        name="mixer",
    )(scalars, mix_input, before, group_weight, pool_gain.reshape(1, -1), branch_weight)


def experts_kernel(scalars, mine, theirs, gate_weight, up_weight, down_weight, members):
    rows, half = mine.shape
    hidden_size = gate_weight.shape[2]
    width = down_weight.shape[2]
    columns = width // members
    chips = members // 2
    inner = half // 4
    half_steps = half // inner
    steps = 2 * half_steps

    def body(scal, mine_ref, theirs_ref, gate_ref, up_ref, down_ref, give_ref, keep_ref, gate, up, hidden):
        step = pl.program_id(0)

        @pl.when(step == 0)
        def _():
            gate[...] = jnp.dot(mine_ref[...], gate_ref[0], preferred_element_type=f32)
            up[...] = jnp.dot(mine_ref[...], up_ref[0], preferred_element_type=f32)

        @pl.when((step > 0) & (step < half_steps))
        def _():
            gate[...] += jnp.dot(mine_ref[...], gate_ref[0], preferred_element_type=f32)
            up[...] += jnp.dot(mine_ref[...], up_ref[0], preferred_element_type=f32)

        @pl.when((step >= half_steps) & (step < steps))
        def _():
            gate[...] += jnp.dot(theirs_ref[...], gate_ref[0], preferred_element_type=f32)
            up[...] += jnp.dot(theirs_ref[...], up_ref[0], preferred_element_type=f32)

        @pl.when(step == steps - 1)
        def _():
            value = gate[...]
            hidden[...] = (value / (1.0 + jnp.exp(-value)) * up[...]).astype(bf16)

        @pl.when((step >= steps) & (step < steps + chips))
        def _():
            give_ref[0] = jnp.dot(hidden[...], down_ref[0], preferred_element_type=f32).astype(bf16)

        @pl.when(step >= steps + chips)
        def _():
            keep_ref[0] = jnp.dot(hidden[...], down_ref[0], preferred_element_type=f32).astype(bf16)

    def weight_at(i, s):
        core = lax.rem(s[0], 2)
        at = jnp.minimum(i, steps - 1)
        own = at < half_steps
        side = jnp.where(own, core, 1 - core)
        return (0, side * half_steps + lax.rem(at, half_steps), 0)

    return pl.pallas_call(
        body,
        grid_spec=pltpu.PrefetchScalarGridSpec(
            num_scalar_prefetch=1,
            grid=(steps + members,),
            in_specs=[
                pl.BlockSpec((rows, inner), lambda i, s: (0, jnp.minimum(i, half_steps - 1))),
                pl.BlockSpec(
                    (rows, inner), lambda i, s: (0, jnp.clip(i - half_steps, 0, half_steps - 1))
                ),
                pl.BlockSpec((1, inner, hidden_size), weight_at),
                pl.BlockSpec((1, inner, hidden_size), weight_at),
                pl.BlockSpec(
                    (1, hidden_size, columns),
                    lambda i, s: (0, 0, column_block(jnp.maximum(i - steps, 0), s[0], chips)),
                ),
            ],
            out_specs=[
                pl.BlockSpec(
                    (1, rows, columns), lambda i, s: (jnp.clip(i - steps, 0, chips - 1), 0, 0)
                ),
                pl.BlockSpec(
                    (1, rows, columns), lambda i, s: (jnp.maximum(i - steps - chips, 0), 0, 0)
                ),
            ],
            scratch_shapes=[
                pltpu.VMEM((rows, hidden_size), f32),
                pltpu.VMEM((rows, hidden_size), f32),
                pltpu.VMEM((rows, hidden_size), bf16),
            ],
        ),
        out_shape=[jax.ShapeDtypeStruct((chips, rows, columns), bf16)] * 2,
        name="experts",
    )(scalars, mine, theirs, gate_weight, up_weight, down_weight)


def reduced(give, keep, cuts):
    chips = give.shape[0]
    got = paired(give)
    pieces = []
    for start, stop in cuts:
        part = [
            (keep[r, start:stop].astype(f32) + got[r, start:stop].astype(f32)).astype(bf16)
            for r in range(chips)
        ]
        total = part[0].astype(f32)
        for r in range(1, chips):
            total = total + rotated(part[r], "tp", 2 * r).astype(f32)
        pieces.append(total.astype(bf16))
    return pieces


def on_device(
    mix_input,
    group_weight,
    pool_gain,
    branch_weight,
    exp_input,
    norm_gain,
    routes,
    route_weights,
    gate_weight,
    up_weight,
    down_weight,
):
    members = lax.axis_size("tp")
    experts = lax.axis_size("ep")
    scalars = jnp.stack([lax.axis_index("tp"), lax.axis_index("ep")]).astype(jnp.int32)
    rows_mix = mix_input.shape[0]
    capacity = 3 * exp_input.shape[0] // experts
    order = sorted(range(1, experts), key=lambda k: -min(k, experts - k)) + [0]
    before = shifted(mix_input[rows_mix - halo :], "ep", 1)
    outgoing = prepare(scalars, exp_input, norm_gain, routes, order, capacity)
    arrivals = [rotated(block, "ep", k) for block, k in zip(outgoing[:-1], order)]
    give, keep = mixer(
        scalars, mix_input, before, group_weight, pool_gain, branch_weight, members
    )
    (mix_out,) = reduced(give, keep, [(0, rows_mix)])
    *arrivals, mix_out = lax.optimization_barrier((*arrivals, mix_out))
    mine = jnp.concatenate([*arrivals, outgoing[-1]], axis=0)
    theirs = paired(mine)
    give, keep = experts_kernel(
        scalars, mine, theirs, gate_weight, up_weight, down_weight, members
    )
    groups = [order[:1], order[1:-1], order[-1:]]
    cuts, at = [], 0
    for group in groups:
        cuts.append((at, at + capacity * len(group)))
        at += capacity * len(group)
    chunks = []
    for group, piece in zip(groups, reduced(give, keep, cuts)):
        for j, k in enumerate(group):
            part = piece[j * capacity : (j + 1) * capacity]
            chunks.append(rotated(part, "ep", -k) if k else part)
    exp_out = combine(scalars, routes, route_weights, chunks, order)
    return (mix_out, exp_out)


def solution(mesh):
    return jax.shard_map(
        on_device,
        mesh=mesh,
        in_specs=(
            P(("grp", "ep"), "tp"),
            P(),
            P(),
            P("tp", None),
            P(("grp", "ep"), None),
            P(),
            P(("grp", "ep"), None),
            P(("grp", "ep"), None),
            P("ep", None, "tp"),
            P("ep", None, "tp"),
            P("ep", "tp", None),
        ),
        out_specs=(P(("grp", "ep"), "tp"), P(("grp", "ep"), "tp")),
        check_vma=False,
    )
```

```python
import jax
import jax.numpy as jnp
from jax import lax
from jax.experimental import pallas as pl
from jax.experimental.pallas import tpu as pltpu
from jax.sharding import PartitionSpec as P

windows = (2, 4, 8, 16)
epsilon = 1e-06
halo = 16
f32, bf16 = jnp.float32, jnp.bfloat16
params = pltpu.CompilerParams(vmem_limit_bytes=24 * 2**20)


def shifted(block, axis, distance):
    devices = range(lax.axis_size(axis))
    route = [(i - distance, i) for i in devices if i - distance in devices]
    return lax.ppermute(block, axis, route)


def rotated(block, axis, distance):
    count = lax.axis_size(axis)
    return lax.ppermute(block, axis, [(i, (i + distance) % count) for i in range(count)])


def paired(block):
    count = lax.axis_size("tp")
    return lax.ppermute(block, "tp", [(i, i ^ 1) for i in range(count)])


def ranks_of(routes, ep_rank, experts):
    tokens, top = routes.shape
    relative = lax.rem(ep_rank + lax.broadcasted_iota(jnp.int32, (tokens, experts), 1), experts)
    hits = [(routes[:, k : k + 1] == relative) for k in range(top)]
    member = sum(jnp.where(h, 1.0, 0.0) for h in hits)
    row = lax.broadcasted_iota(jnp.int32, (tokens, tokens), 0)
    col = lax.broadcasted_iota(jnp.int32, (tokens, tokens), 1)
    before = jnp.where(col < row, 1.0, 0.0).astype(bf16)
    rank = jnp.dot(before, member.astype(bf16), preferred_element_type=f32)
    return [jnp.where(h, rank, -1.0) for h in hits], jnp.where(member > 0.5, rank, -1.0)


def prepare(scalars, exp_input, norm_gain, routes, order, capacity):
    tokens, width = exp_input.shape
    half = width // 2
    experts = len(order)
    top = routes.shape[1]

    def body(scal, x_ref, gain_ref, routes_ref, *outs):
        floated = x_ref[...].astype(f32)
        scale = lax.rsqrt(jnp.mean(floated * floated, axis=1, keepdims=True) + epsilon)
        low = (floated[:, :half] * scale * gain_ref[:, :half]).astype(bf16)
        high = (floated[:, half:] * scale * gain_ref[:, half:]).astype(bf16)
        mine = jnp.where(lax.rem(scal[0], 2) == 0, low, high)
        relative = lax.rem(
            scal[1] + lax.broadcasted_iota(jnp.int32, (experts, tokens), 0), experts
        )
        member = sum(
            jnp.where(routes_ref[k : k + 1, :] == relative, 1.0, 0.0) for k in range(top)
        )
        row = lax.broadcasted_iota(jnp.int32, (tokens, tokens), 0)
        col = lax.broadcasted_iota(jnp.int32, (tokens, tokens), 1)
        earlier = jnp.where(row < col, 1.0, 0.0).astype(bf16)
        rank = jnp.dot(member.astype(bf16), earlier, preferred_element_type=f32)
        place = jnp.where(member > 0.5, rank, -1.0)
        slots = lax.broadcasted_iota(jnp.int32, (capacity, tokens), 0).astype(f32)
        for out, k in zip(outs, order):
            pick = jnp.where(place[k : k + 1, :] == slots, 1.0, 0.0).astype(bf16)
            out[...] = jnp.dot(pick, mine, preferred_element_type=f32).astype(bf16)

    return pl.pallas_call(
        body,
        in_specs=[
            pl.BlockSpec(memory_space=pltpu.SMEM),
            pl.BlockSpec(memory_space=pltpu.VMEM),
            pl.BlockSpec(memory_space=pltpu.VMEM),
            pl.BlockSpec(memory_space=pltpu.VMEM),
        ],
        out_specs=[pl.BlockSpec(memory_space=pltpu.VMEM)] * experts,
        out_shape=[jax.ShapeDtypeStruct((capacity, half), bf16)] * experts,
        name="prepare",
        compiler_params=params,
    )(scalars, exp_input, norm_gain.reshape(1, width), routes.T)


def combine(scalars, routes, route_weights, chunks, order):
    tokens, top = routes.shape
    capacity, columns = chunks[0].shape
    experts = len(order)

    def body(scal, routes_ref, weights_ref, *refs):
        out = refs[-1]
        places, _ = ranks_of(routes_ref[...], scal[1], experts)
        slots = lax.broadcasted_iota(jnp.int32, (tokens, capacity), 1).astype(f32)
        total = jnp.zeros((tokens, columns), f32)
        for k in range(top):
            chosen = jnp.zeros((tokens, columns), f32)
            for ref, e in zip(refs, order):
                pick = jnp.where(places[k][:, e : e + 1] == slots, 1.0, 0.0).astype(bf16)
                chosen = chosen + jnp.dot(pick, ref[...], preferred_element_type=f32)
            total = total + chosen * weights_ref[:, k : k + 1]
        out[...] = total.astype(bf16)

    return pl.pallas_call(
        body,
        in_specs=[pl.BlockSpec(memory_space=pltpu.SMEM)]
        + [pl.BlockSpec(memory_space=pltpu.VMEM)] * (2 + experts),
        out_specs=pl.BlockSpec(memory_space=pltpu.VMEM),
        out_shape=jax.ShapeDtypeStruct((tokens, columns), bf16),
        name="combine",
        compiler_params=params,
    )(scalars, routes, route_weights, *chunks)


def column_block(step, rank, chips):
    core, chip = lax.rem(rank, 2), lax.div(rank, 2)
    place = lax.rem(chip + step % chips, chips)
    return 2 * place + (1 - core if step < chips else core)


def mixer(scalars, mix_input, before, group_weight, pool_gain, branch_weight, members):
    rows, channels = mix_input.shape
    group_width = group_weight.shape[1]
    group_count = channels // group_width
    width = branch_weight.shape[1]
    columns = width // members
    chips = members // 2

    def body(scal, x_hbm, before_ref, group_hbm, gain_ref, branch_hbm, give_ref, keep_ref,
             x_ref, group_ref, branch_ref, pooled, sems):
        copies = [
            pltpu.make_async_copy(x_hbm, x_ref, sems.at[0]),
            pltpu.make_async_copy(
                group_hbm.at[pl.ds(scal[0] * group_count, group_count)], group_ref, sems.at[1]
            ),
            pltpu.make_async_copy(branch_hbm, branch_ref, sems.at[2]),
        ]
        for copy in copies:
            copy.start()
        copies[0].wait()
        copies[1].wait()
        place = scal[1] * rows + lax.broadcasted_iota(jnp.int32, (rows, group_width), 0)
        for g in range(group_count):
            cut = slice(g * group_width, (g + 1) * group_width)
            extended = jnp.concatenate(
                [before_ref[:, cut].astype(f32), x_ref[:, cut].astype(f32)], axis=0
            )
            level = lax.rem(scal[0] * group_count + g, len(windows))
            sums = extended
            chosen = jnp.zeros_like(extended)
            for index, window in enumerate(windows):
                sums = sums + pltpu.roll(sums, window // 2, 0)
                chosen = jnp.where(level == index, sums, chosen)
            length = lax.shift_left(jnp.int32(2), level)
            counted = jnp.minimum(place + 1, length).astype(f32)
            deviation = (chosen[halo:] / counted - extended[halo:]).astype(bf16)
            grouped = jnp.dot(deviation, group_ref[g], preferred_element_type=f32)
            at = pl.multiple_of(scal[0] * channels + g * group_width, 128)
            pooled[:, cut] = (grouped * gain_ref[:, pl.ds(at, group_width)]).astype(bf16)
        copies[2].wait()
        for step in range(members):
            at = pl.multiple_of(column_block(step, scal[0], chips) * columns, 128)
            result = jnp.dot(
                pooled[...], branch_ref[:, pl.ds(at, columns)], preferred_element_type=f32
            ).astype(bf16)
            if step < chips:
                give_ref[step] = result
            else:
                keep_ref[step - chips] = result

    vmem = pl.BlockSpec(memory_space=pltpu.VMEM)
    hbm = pl.BlockSpec(memory_space=pltpu.HBM)
    return pl.pallas_call(
        body,
        in_specs=[pl.BlockSpec(memory_space=pltpu.SMEM), hbm, vmem, hbm, vmem, hbm],
        out_specs=[vmem, vmem],
        scratch_shapes=[
            pltpu.VMEM((rows, channels), bf16),
            pltpu.VMEM((group_count, group_width, group_width), bf16),
            pltpu.VMEM(branch_weight.shape, bf16),
            pltpu.VMEM((rows, channels), bf16),
            pltpu.SemaphoreType.DMA((3,)),
        ],
        out_shape=[jax.ShapeDtypeStruct((chips, rows, columns), bf16)] * 2,
        name="mixer",
        compiler_params=params,
    )(scalars, mix_input, before, group_weight, pool_gain.reshape(1, -1), branch_weight)


def load(*weights):
    count = len(weights)

    def body(*refs):
        sems = refs[-1]
        copies = [
            pltpu.make_async_copy(refs[i], refs[count + i], sems.at[i]) for i in range(count)
        ]
        for copy in copies:
            copy.start()
        for copy in copies:
            copy.wait()

    return pl.pallas_call(
        body,
        in_specs=[pl.BlockSpec(memory_space=pltpu.HBM)] * count,
        out_specs=[pl.BlockSpec(memory_space=pl.ANY)] * count,
        out_shape=[jax.ShapeDtypeStruct(w.shape, w.dtype) for w in weights],
        scratch_shapes=[pltpu.SemaphoreType.DMA((count,))],
        name="load",
        compiler_params=params,
    )(*weights)


def whole_call(body, shapes, scalars, *arrays):
    vmem = pl.BlockSpec(memory_space=pltpu.VMEM)
    return pl.pallas_call(
        body,
        in_specs=[pl.BlockSpec(memory_space=pltpu.SMEM)] + [vmem] * len(arrays),
        out_specs=[vmem] * len(shapes),
        out_shape=shapes,
        compiler_params=params,
    )(scalars, *arrays)


def enter(scalars, mine, gate_weight, up_weight):
    rows, half = mine.shape
    shape = jax.ShapeDtypeStruct((rows, gate_weight.shape[2]), f32)

    def body(scal, mine_ref, gate_ref, up_ref, gate, up):
        at = pl.ds(pl.multiple_of(lax.rem(scal[0], 2) * half, 128), half)
        gate[...] = jnp.dot(mine_ref[...], gate_ref[0, at, :], preferred_element_type=f32)
        up[...] = jnp.dot(mine_ref[...], up_ref[0, at, :], preferred_element_type=f32)

    return whole_call(body, [shape, shape], scalars, mine, gate_weight, up_weight)


def middle(scalars, theirs, gate_weight, up_weight, gate, up, down_weight, members):
    rows, half = theirs.shape
    hidden_size, width = down_weight.shape[1:]
    columns, chips = width // members, members // 2

    def body(scal, theirs_ref, gate_ref, up_ref, gate_acc, up_acc, down_ref, hidden, give):
        at = pl.ds(pl.multiple_of((1 - lax.rem(scal[0], 2)) * half, 128), half)
        value = gate_acc[...] + jnp.dot(
            theirs_ref[...], gate_ref[0, at, :], preferred_element_type=f32
        )
        other = up_acc[...] + jnp.dot(
            theirs_ref[...], up_ref[0, at, :], preferred_element_type=f32
        )
        hidden[...] = (value / (1.0 + jnp.exp(-value)) * other).astype(bf16)
        for step in range(chips):
            col = pl.multiple_of(column_block(step, scal[0], chips) * columns, 128)
            give[step] = jnp.dot(
                hidden[...], down_ref[0, :, pl.ds(col, columns)], preferred_element_type=f32
            ).astype(bf16)

    shapes = [
        jax.ShapeDtypeStruct((rows, hidden_size), bf16),
        jax.ShapeDtypeStruct((chips, rows, columns), bf16),
    ]
    return whole_call(body, shapes, scalars, theirs, gate_weight, up_weight, gate, up, down_weight)


def leave(scalars, hidden, down_weight, members):
    rows = hidden.shape[0]
    columns, chips = down_weight.shape[2] // members, members // 2

    def body(scal, hidden_ref, down_ref, keep):
        for step in range(chips):
            col = pl.multiple_of(column_block(chips + step, scal[0], chips) * columns, 128)
            keep[step] = jnp.dot(
                hidden_ref[...], down_ref[0, :, pl.ds(col, columns)], preferred_element_type=f32
            ).astype(bf16)

    shape = jax.ShapeDtypeStruct((chips, rows, columns), bf16)
    return whole_call(body, [shape], scalars, hidden, down_weight)[0]


def reduced(got, keep, cuts):
    chips = keep.shape[0]
    pieces = []
    for start, stop in cuts:
        part = [
            (keep[r, start:stop].astype(f32) + got[r, start:stop].astype(f32)).astype(bf16)
            for r in range(chips)
        ]
        total = part[0].astype(f32)
        for r in range(1, chips):
            moved = rotated(part[r], "tp", 2 * r)
            total = total + moved.astype(f32)
        pieces.append(total.astype(bf16))
    return pieces


def layer(
    mix_input,
    group_weight,
    pool_gain,
    branch_weight,
    exp_input,
    norm_gain,
    routes,
    route_weights,
    gate_weight,
    up_weight,
    down_weight,
):
    members = lax.axis_size("tp")
    experts = lax.axis_size("ep")
    scalars = jnp.stack([lax.axis_index("tp"), lax.axis_index("ep")]).astype(jnp.int32)
    rows_mix = mix_input.shape[0]
    capacity = 3 * exp_input.shape[0] // experts
    order = sorted(range(1, experts), key=lambda k: -min(k, experts - k)) + [0]
    outgoing = prepare(scalars, exp_input, norm_gain, routes, order, capacity)
    *outgoing, late_mix = lax.optimization_barrier((*outgoing, mix_input))
    arrivals = []
    for block, k in zip(outgoing[:-1], order):
        arrivals.append(rotated(block, "ep", k))
    before = shifted(late_mix[rows_mix - halo :], "ep", 1)
    give, keep = mixer(scalars, mix_input, before, group_weight, pool_gain, branch_weight, members)
    got = paired(give)
    (mix_out,) = reduced(got, keep, [(0, rows_mix)])
    gate_weight, up_weight, down_weight = load(gate_weight, up_weight, down_weight)
    *arrivals, mix_out = lax.optimization_barrier((*arrivals, mix_out))
    mine = jnp.concatenate([*arrivals, outgoing[-1]], axis=0)
    theirs = paired(mine)
    gate, up = enter(scalars, mine, gate_weight, up_weight)
    hidden, give = middle(scalars, theirs, gate_weight, up_weight, gate, up, down_weight, members)
    got = paired(give)
    keep = leave(scalars, hidden, down_weight, members)
    groups = [order[:1], order[1:-1], order[-1:]]
    cuts, at = [], 0
    for group in groups:
        cuts.append((at, at + capacity * len(group)))
        at += capacity * len(group)
    chunks = []
    for group, piece in zip(groups, reduced(got, keep, cuts)):
        for j, k in enumerate(group):
            part = piece[j * capacity : (j + 1) * capacity]
            chunks.append(rotated(part, "ep", -k) if k else part)
    exp_out = combine(scalars, routes, route_weights, chunks, order)
    return (mix_out, exp_out)


def solution(mesh):
    return jax.shard_map(
        layer,
        mesh=mesh,
        in_specs=(
            P(("grp", "ep"), "tp"),
            P(),
            P(),
            P("tp", None),
            P(("grp", "ep"), None),
            P(),
            P(("grp", "ep"), None),
            P(("grp", "ep"), None),
            P("ep", None, "tp"),
            P("ep", None, "tp"),
            P("ep", "tp", None),
        ),
        out_specs=(P(("grp", "ep"), "tp"), P(("grp", "ep"), "tp")),
        check_vma=False,
    )
```

```python
import jax
import jax.numpy as jnp
from jax import lax
from jax.experimental import pallas as pl
from jax.experimental.pallas import tpu as pltpu
from jax.sharding import PartitionSpec as P

windows = (2, 4, 8, 16)
epsilon = 1e-06
halo = 16
f32, bf16 = jnp.float32, jnp.bfloat16
params = pltpu.CompilerParams(vmem_limit_bytes=24 * 2**20)


def rotated(block, axis, distance):
    count = lax.axis_size(axis)
    return lax.ppermute(block, axis, [(i, (i + distance) % count) for i in range(count)])


def paired(block):
    count = lax.axis_size("tp")
    return lax.ppermute(block, "tp", [(i, i ^ 1) for i in range(count)])


def ranks_of(routes, ep_rank, experts):
    tokens, top = routes.shape
    relative = lax.rem(ep_rank + lax.broadcasted_iota(jnp.int32, (tokens, experts), 1), experts)
    hits = [(routes[:, k : k + 1] == relative) for k in range(top)]
    member = sum(jnp.where(h, 1.0, 0.0) for h in hits)
    row = lax.broadcasted_iota(jnp.int32, (tokens, tokens), 0)
    col = lax.broadcasted_iota(jnp.int32, (tokens, tokens), 1)
    before = jnp.where(col < row, 1.0, 0.0).astype(bf16)
    rank = jnp.dot(before, member.astype(bf16), preferred_element_type=f32)
    return [jnp.where(h, rank, -1.0) for h in hits], jnp.where(member > 0.5, rank, -1.0)


def prepare(scalars, exp_input, norm_gain, routes, order, capacity):
    tokens, width = exp_input.shape
    half = width // 2
    experts = len(order)
    top = routes.shape[1]

    def body(scal, x_ref, gain_ref, routes_ref, *outs):
        floated = x_ref[...].astype(f32)
        scale = lax.rsqrt(jnp.mean(floated * floated, axis=1, keepdims=True) + epsilon)
        low = (floated[:, :half] * scale * gain_ref[:, :half]).astype(bf16)
        high = (floated[:, half:] * scale * gain_ref[:, half:]).astype(bf16)
        mine = jnp.where(lax.rem(scal[0], 2) == 0, low, high)
        relative = lax.rem(
            scal[1] + lax.broadcasted_iota(jnp.int32, (experts, tokens), 0), experts
        )
        member = sum(
            jnp.where(routes_ref[k : k + 1, :] == relative, 1.0, 0.0) for k in range(top)
        )
        row = lax.broadcasted_iota(jnp.int32, (tokens, tokens), 0)
        col = lax.broadcasted_iota(jnp.int32, (tokens, tokens), 1)
        earlier = jnp.where(row < col, 1.0, 0.0).astype(bf16)
        rank = jnp.dot(member.astype(bf16), earlier, preferred_element_type=f32)
        place = jnp.where(member > 0.5, rank, -1.0)
        slots = lax.broadcasted_iota(jnp.int32, (capacity, tokens), 0).astype(f32)
        for out, k in zip(outs, order):
            pick = jnp.where(place[k : k + 1, :] == slots, 1.0, 0.0).astype(bf16)
            out[...] = jnp.dot(pick, mine, preferred_element_type=f32).astype(bf16)

    return pl.pallas_call(
        body,
        in_specs=[
            pl.BlockSpec(memory_space=pltpu.SMEM),
            pl.BlockSpec(memory_space=pltpu.VMEM),
            pl.BlockSpec(memory_space=pltpu.VMEM),
            pl.BlockSpec(memory_space=pltpu.VMEM),
        ],
        out_specs=[pl.BlockSpec(memory_space=pltpu.VMEM)] * experts,
        out_shape=[jax.ShapeDtypeStruct((capacity, half), bf16)] * experts,
        name="prepare",
        compiler_params=params,
    )(scalars, exp_input, norm_gain.reshape(1, width), routes.T)


def picks_of(scalars, routes, capacity, order):
    tokens, top = routes.shape
    experts = len(order)

    def body(scal, routes_ref, *outs):
        places, _ = ranks_of(routes_ref[...], scal[1], experts)
        slots = lax.broadcasted_iota(jnp.int32, (tokens, capacity), 1).astype(f32)
        for out, e in zip(outs, order):
            for k in range(top):
                out[k * tokens : (k + 1) * tokens] = jnp.where(
                    places[k][:, e : e + 1] == slots, 1.0, 0.0
                ).astype(bf16)

    shape = jax.ShapeDtypeStruct((top * tokens, capacity), bf16)
    return whole_call(body, [shape] * experts, scalars, routes)


def combine(scalars, picks, route_weights, chunks):
    tokens, top = route_weights.shape
    columns = chunks[0].shape[1]
    count = len(chunks)

    def body(scal, weights_ref, *refs):
        chosen = jnp.zeros((top * tokens, columns), f32)
        for pick, chunk in zip(refs[:count], refs[count:-1]):
            chosen = chosen + jnp.dot(pick[...], chunk[...], preferred_element_type=f32)
        total = jnp.zeros((tokens, columns), f32)
        for k in range(top):
            total = total + chosen[k * tokens : (k + 1) * tokens] * weights_ref[:, k : k + 1]
        refs[-1][...] = total.astype(bf16)

    shape = jax.ShapeDtypeStruct((tokens, columns), bf16)
    return whole_call(body, [shape], scalars, route_weights, *picks, *chunks)[0]


def column_block(step, rank, chips):
    core, chip = lax.rem(rank, 2), lax.div(rank, 2)
    place = lax.rem(chip + step % chips, chips)
    return 2 * place + (1 - core if step < chips else core)


def mixer(scalars, mix_input, before, group_weight, pool_gain, branch_weight, members):
    rows, channels = mix_input.shape
    group_width = group_weight.shape[1]
    group_count = channels // group_width
    width = branch_weight.shape[1]
    columns = width // members
    chips = members // 2

    def body(scal, x_hbm, before_ref, group_hbm, gain_ref, branch_hbm, give_ref, keep_ref,
             x_ref, group_ref, branch_ref, pooled, sems):
        copies = [
            pltpu.make_async_copy(x_hbm, x_ref, sems.at[0]),
            pltpu.make_async_copy(
                group_hbm.at[pl.ds(scal[0] * group_count, group_count)], group_ref, sems.at[1]
            ),
            pltpu.make_async_copy(branch_hbm, branch_ref, sems.at[2]),
        ]
        for copy in copies:
            copy.start()
        copies[0].wait()
        copies[1].wait()
        place = scal[1] * rows + lax.broadcasted_iota(jnp.int32, (rows, group_width), 0)
        for g in range(group_count):
            cut = slice(g * group_width, (g + 1) * group_width)
            earlier = jnp.where(scal[1] > 0, before_ref[:, cut].astype(f32), 0.0)
            extended = jnp.concatenate([earlier, x_ref[:, cut].astype(f32)], axis=0)
            level = lax.rem(scal[0] * group_count + g, len(windows))
            sums = extended
            chosen = jnp.zeros_like(extended)
            for index, window in enumerate(windows):
                sums = sums + pltpu.roll(sums, window // 2, 0)
                chosen = jnp.where(level == index, sums, chosen)
            length = lax.shift_left(jnp.int32(2), level)
            counted = jnp.minimum(place + 1, length).astype(f32)
            deviation = (chosen[halo:] / counted - extended[halo:]).astype(bf16)
            grouped = jnp.dot(deviation, group_ref[g], preferred_element_type=f32)
            at = pl.multiple_of(scal[0] * channels + g * group_width, 128)
            pooled[:, cut] = (grouped * gain_ref[:, pl.ds(at, group_width)]).astype(bf16)
        copies[2].wait()
        for step in range(members):
            at = pl.multiple_of(column_block(step, scal[0], chips) * columns, 128)
            result = jnp.dot(
                pooled[...], branch_ref[:, pl.ds(at, columns)], preferred_element_type=f32
            ).astype(bf16)
            if step < chips:
                give_ref[step] = result
            else:
                keep_ref[step - chips] = result

    vmem = pl.BlockSpec(memory_space=pltpu.VMEM)
    hbm = pl.BlockSpec(memory_space=pltpu.HBM)
    return pl.pallas_call(
        body,
        in_specs=[pl.BlockSpec(memory_space=pltpu.SMEM), hbm, vmem, hbm, vmem, hbm],
        out_specs=[vmem, vmem],
        scratch_shapes=[
            pltpu.VMEM((rows, channels), bf16),
            pltpu.VMEM((group_count, group_width, group_width), bf16),
            pltpu.VMEM(branch_weight.shape, bf16),
            pltpu.VMEM((rows, channels), bf16),
            pltpu.SemaphoreType.DMA((3,)),
        ],
        out_shape=[jax.ShapeDtypeStruct((chips, rows, columns), bf16)] * 2,
        name="mixer",
        compiler_params=params,
    )(scalars, mix_input, before, group_weight, pool_gain.reshape(1, -1), branch_weight)


def load(*weights):
    count = len(weights)

    def body(*refs):
        sems = refs[-1]
        copies = [
            pltpu.make_async_copy(refs[i], refs[count + i], sems.at[i]) for i in range(count)
        ]
        for copy in copies:
            copy.start()
        for copy in copies:
            copy.wait()

    return pl.pallas_call(
        body,
        in_specs=[pl.BlockSpec(memory_space=pltpu.HBM)] * count,
        out_specs=[pl.BlockSpec(memory_space=pl.ANY)] * count,
        out_shape=[jax.ShapeDtypeStruct(w.shape, w.dtype) for w in weights],
        scratch_shapes=[pltpu.SemaphoreType.DMA((count,))],
        name="load",
        compiler_params=params,
    )(*weights)


def whole_call(body, shapes, scalars, *arrays):
    vmem = pl.BlockSpec(memory_space=pltpu.VMEM)
    return pl.pallas_call(
        body,
        in_specs=[pl.BlockSpec(memory_space=pltpu.SMEM)] + [vmem] * len(arrays),
        out_specs=[vmem] * len(shapes),
        out_shape=shapes,
        compiler_params=params,
    )(scalars, *arrays)


def enter(scalars, mine, gate_weight, up_weight):
    rows, half = mine.shape
    shape = jax.ShapeDtypeStruct((rows, gate_weight.shape[2]), f32)

    def body(scal, mine_ref, gate_ref, up_ref, gate, up):
        at = pl.ds(pl.multiple_of(lax.rem(scal[0], 2) * half, 128), half)
        gate[...] = jnp.dot(mine_ref[...], gate_ref[0, at, :], preferred_element_type=f32)
        up[...] = jnp.dot(mine_ref[...], up_ref[0, at, :], preferred_element_type=f32)

    return whole_call(body, [shape, shape], scalars, mine, gate_weight, up_weight)


def middle(scalars, theirs, gate_weight, up_weight, gate, up, down_weight, members):
    rows, half = theirs.shape
    hidden_size, width = down_weight.shape[1:]
    columns, chips = width // members, members // 2

    def body(scal, theirs_ref, gate_ref, up_ref, gate_acc, up_acc, down_ref, hidden, give):
        at = pl.ds(pl.multiple_of((1 - lax.rem(scal[0], 2)) * half, 128), half)
        value = gate_acc[...] + jnp.dot(
            theirs_ref[...], gate_ref[0, at, :], preferred_element_type=f32
        )
        other = up_acc[...] + jnp.dot(
            theirs_ref[...], up_ref[0, at, :], preferred_element_type=f32
        )
        hidden[...] = (value / (1.0 + jnp.exp(-value)) * other).astype(bf16)
        for step in range(chips):
            col = pl.multiple_of(column_block(step, scal[0], chips) * columns, 128)
            give[step] = jnp.dot(
                hidden[...], down_ref[0, :, pl.ds(col, columns)], preferred_element_type=f32
            ).astype(bf16)

    shapes = [
        jax.ShapeDtypeStruct((rows, hidden_size), bf16),
        jax.ShapeDtypeStruct((chips, rows, columns), bf16),
    ]
    return whole_call(body, shapes, scalars, theirs, gate_weight, up_weight, gate, up, down_weight)


def leave(scalars, hidden, down_weight, members):
    rows = hidden.shape[0]
    columns, chips = down_weight.shape[2] // members, members // 2

    def body(scal, hidden_ref, down_ref, keep):
        for step in range(chips):
            col = pl.multiple_of(column_block(chips + step, scal[0], chips) * columns, 128)
            keep[step] = jnp.dot(
                hidden_ref[...], down_ref[0, :, pl.ds(col, columns)], preferred_element_type=f32
            ).astype(bf16)

    shape = jax.ShapeDtypeStruct((chips, rows, columns), bf16)
    return whole_call(body, [shape], scalars, hidden, down_weight)[0]


def reduced(got, keep, cuts):
    chips = keep.shape[0]
    pieces = []
    for index, (start, stop) in enumerate(cuts):
        if index:
            got, keep = lax.optimization_barrier((got, keep))
        part = [
            (keep[r, start:stop].astype(f32) + got[r, start:stop].astype(f32)).astype(bf16)
            for r in range(chips)
        ]
        total = part[0].astype(f32)
        for r in range(1, chips):
            moved = rotated(part[r], "tp", 2 * r)
            total = total + moved.astype(f32)
        pieces.append(total.astype(bf16))
    return pieces


def layer(
    mix_input,
    group_weight,
    pool_gain,
    branch_weight,
    exp_input,
    norm_gain,
    routes,
    route_weights,
    gate_weight,
    up_weight,
    down_weight,
):
    members = lax.axis_size("tp")
    experts = lax.axis_size("ep")
    scalars = jnp.stack([lax.axis_index("tp"), lax.axis_index("ep")]).astype(jnp.int32)
    rows_mix = mix_input.shape[0]
    capacity = 3 * exp_input.shape[0] // experts
    order = sorted(range(1, experts), key=lambda k: -min(k, experts - k)) + [0]
    outgoing = prepare(scalars, exp_input, norm_gain, routes, order, capacity)
    *outgoing, late_mix = lax.optimization_barrier((*outgoing, mix_input))
    arrivals = []
    for block, k in zip(outgoing[:-1], order):
        arrivals.append(rotated(block, "ep", k))
    before = rotated(late_mix[rows_mix - halo :], "ep", 1)
    give, keep = mixer(scalars, mix_input, before, group_weight, pool_gain, branch_weight, members)
    got = paired(give)
    (mix_out,) = reduced(got, keep, [(0, rows_mix)])
    gate_weight, up_weight, down_weight = load(gate_weight, up_weight, down_weight)
    mine = jnp.concatenate([*arrivals, outgoing[-1]], axis=0)
    theirs = paired(mine)
    gate, up = enter(scalars, mine, gate_weight, up_weight)
    hidden, give = middle(scalars, theirs, gate_weight, up_weight, gate, up, down_weight, members)
    got = paired(give)
    keep = leave(scalars, hidden, down_weight, members)
    picks = picks_of(scalars, routes, capacity, order)
    groups = [order[:1], order[1:-1], order[-1:]]
    cuts, at = [], 0
    for group in groups:
        cuts.append((at, at + capacity * len(group)))
        at += capacity * len(group)
    chunks = []
    for group, piece in zip(groups, reduced(got, keep, cuts)):
        for j, k in enumerate(group):
            part = piece[j * capacity : (j + 1) * capacity]
            chunks.append(rotated(part, "ep", -k) if k else part)
    exp_out = combine(scalars, picks, route_weights, chunks)
    return (mix_out, exp_out)


def solution(mesh):
    return jax.shard_map(
        layer,
        mesh=mesh,
        in_specs=(
            P(("grp", "ep"), "tp"),
            P(),
            P(),
            P("tp", None),
            P(("grp", "ep"), None),
            P(),
            P(("grp", "ep"), None),
            P(("grp", "ep"), None),
            P("ep", None, "tp"),
            P("ep", None, "tp"),
            P("ep", "tp", None),
        ),
        out_specs=(P(("grp", "ep"), "tp"), P(("grp", "ep"), "tp")),
        check_vma=False,
    )
```
